32 devices in a mesh: sp: 8 (over z, y), tp: 4 (over x, core).
Axes of the slice: x: 2, y: 2, z: 4, core: 2. Of those that a mesh axis runs over, the one named last changes fastest.
Arguments:
- moe_input: bfloat16 [2048, 2048], P('sp'), may hold values from -17.5 to 17.5
- cotangent: bfloat16 [2048, 2048], P('sp'), may hold values from -6 to 6
- routes: int32 [2048, 2], P('sp'), may hold values from 0 to 7, all different within a row; in each aligned block of 256 rows (0 to 255, 256 to 511, ...) at most 80 rows name the same one
- route_weights: float32 [2048, 2], P('sp'), may hold values from 0.2 to 1
- gate_weight: bfloat16 [8, 2048, 2048], P('sp', None, 'tp'), may hold values from -0.125 to 0.125
- up_weight: bfloat16 [8, 2048, 2048], P('sp', None, 'tp'), may hold values from -0.125 to 0.125
- down_weight: bfloat16 [8, 2048, 2048], P('sp', 'tp'), may hold values from -0.125 to 0.125
- out_weight: bfloat16 [2048, 2048], P(None, 'tp'), may hold values from -0.125 to 0.125
- mixer_output: bfloat16 [2048, 2048], P('sp', 'tp'), may hold values from -6 to 6
- queries: bfloat16 [2048, 2048], P('sp', 'tp'), may hold values from -6 to 6
- key_vectors: bfloat16 [2048, 2048], P('sp', 'tp'), may hold values from -0.75 to 0.75
- value_vectors: bfloat16 [2048, 2048], P('sp', 'tp'), may hold values from -6 to 6
- log_decay: float32 [2048, 32], P('sp', 'tp'), may hold values from -0.85 to 0
- block_states: bfloat16 [16, 32, 64, 64], P('sp', 'tp'), may hold values from -1.5 to 1.5
Outputs:
- grad_gate: float32 [8, 2048, 2048], P('sp', None, 'tp')
- grad_up: float32 [8, 2048, 2048], P('sp', None, 'tp')
- grad_down: float32 [8, 2048, 2048], P('sp', 'tp')
- grad_out: float32 [2048, 2048], P('sp', 'tp')
- grad_queries: bfloat16 [2048, 2048], P('sp', 'tp')
- grad_keys: bfloat16 [2048, 2048], P('sp', 'tp')
- grad_values: bfloat16 [2048, 2048], P('sp', 'tp')
The draws below stay inside these ranges and needn't reach their ends.
Inputs may be any that keep to these rules, and one draw needn't show every extreme that they name: `routes`: each row names 2 different experts. Among the rows of one device no expert is named by more than 80 rows, and in every draw some device's rows name some expert exactly 80 times.
All inputs are finite; a program needn't handle non-finite values.
Results may differ from the reference program's by a relative error of at most 0.02.
Values may be sent and summed in bfloat16 or wider, within the bound.
No kernel may reach another device: no remote copies, remote signals or barrier semaphores. Data moves between devices by JAX's collectives and lax.ppermute only.
A program may use at most 128 MiB of HBM per device.

```python
import math
import jax
import jax.numpy as jnp
import numpy as np
from jax import lax

D = 2048
FF = 2048
HEADS = 32
HEAD_DIM = 64
EXPERTS = 8
TOP_K = 2
TOK_DEV = 256
TOKENS = 2048
CAP = 80
BLK = 128
NBLK = 16
N_SP = 8
N_TP = 4


def draw_moe_input(key, part):
    key_rows, key_values = jax.random.split(key)
    row_scale = jnp.exp(jax.random.uniform(key_rows, (TOKENS, 1), jnp.float32, jnp.log(0.25), jnp.log(3.0)))
    values = jnp.clip(jax.random.normal(key_values, (TOKENS, D), jnp.float32), -3.5, 3.5)
    return (values * row_scale).astype(jnp.bfloat16)


def draw_log_decay(key, part):
    subkeys = jax.random.split(key, 9)
    fast_edge = 0.3
    middle_edge = 0.55
    head_class = jax.random.uniform(subkeys[0], (HEADS,), jnp.float32)
    fast_rate = jax.random.uniform(subkeys[1], (HEADS,), jnp.float32, 1.0 / 50.0, 1.0 / 30.0)
    middle_rate = jnp.exp(jax.random.uniform(subkeys[8], (HEADS,), jnp.float32, jnp.log(1.0 / 2048.0), jnp.log(1.0 / 256.0)))
    chain_rate = jax.random.uniform(subkeys[2], (HEADS,), jnp.float32, 0.05, 0.15) / TOKENS
    base_rate = jnp.where(head_class < fast_edge, fast_rate, jnp.where(head_class < middle_edge, middle_rate, chain_rate))
    segment_factor = jax.random.uniform(subkeys[3], (TOKENS // TOK_DEV, 1, HEADS), jnp.float32, 1.0, 3.0)
    jitter = jax.random.uniform(subkeys[4], (TOKENS // TOK_DEV, TOK_DEV, HEADS), jnp.float32, 0.5, 1.5)
    forgetting_factor_matrix = (segment_factor * jitter).reshape(TOKENS, HEADS) * base_rate[None, :]
    primary_expert_index = jax.random.randint(subkeys[5], (HEADS,), 0, TOKENS)
    runner_expert_index = (primary_expert_index + 1 + jax.random.randint(subkeys[6], (HEADS,), 0, TOKENS - 1)) % TOKENS
    discarded_log_terms = jnp.log(jax.random.uniform(subkeys[7], (2, HEADS), jnp.float32, 0.5, 0.8))
    sequence_indices = jnp.arange(TOKENS, dtype=jnp.int32)[:, None]
    exchange_batches = jnp.where(sequence_indices == primary_expert_index[None, :], discarded_log_terms[0][None, :], 0.0)
    exchange_batches = exchange_batches + jnp.where(sequence_indices == runner_expert_index[None, :], discarded_log_terms[1][None, :], 0.0)
    return (exchange_batches - forgetting_factor_matrix).astype(jnp.float32)


def spiked(values, own_key, source, target, shards_of, factor):
    owner, partner = [(jnp.arange(values.shape[axis_at]) // (values.shape[axis_at] // shards_of)).reshape([-1 if axis == axis_at else 1 for axis in range(values.ndim)]) for axis_at in (source, target)]
    chosen = jax.random.permutation(own_key, shards_of)[partner]
    strong = (owner == chosen) | (owner == (partner + shards_of // 2) % shards_of)
    return jnp.where(strong, factor * values, values)


def level_of(rng, shape, cuts, low, top_value):
    loudness, own = 1.0, jax.random.fold_in(rng, 6)
    for position, shards_of in cuts:
        heights = jnp.exp(jax.random.uniform(jax.random.fold_in(own, position), (shards_of,), jnp.float32, low / len(cuts), top_value / len(cuts)))
        loudness = loudness * jnp.repeat(heights, shape[position] // shards_of).reshape([-1 if axis == position else 1 for axis in range(len(shape))])
    return loudness


def deal_out(own_key, own, number, rows, count, top, reach, slope):
    sequence = jax.random.permutation(own_key, count)
    packed, usual = shares(count, rows * top, reach, slope, True), shares(count, rows * top, reach, slope, False)
    places = jnp.arange(count)

    def named(lengths, offset_by):
        used = int((lengths > 0).sum())
        fixed = max(1, used // 4)
        passed = fixed + (places - fixed + offset_by * (used - fixed)) % max(1, count - fixed)
        return jnp.zeros((count,), jnp.int32).at[sequence[jnp.where(places < fixed, places, passed)]].set(jnp.asarray(lengths, jnp.int32))

    lengths = jnp.where(number % 4 == 0, named(packed, number // 4), named(usual, number - number // 4 - 1))
    mixed = jax.random.permutation(jax.random.fold_in(own, 3), count)
    donor, receiver = mixed[0:count // 2 * 2:2], mixed[1:count // 2 * 2:2]
    room = jnp.minimum(lengths[donor] - 1, reach - lengths[receiver]) // 2
    room = jnp.where((donor == sequence[0]) | (receiver == sequence[0]) | (lengths[receiver] == 0), 0, jnp.maximum(room, 0))
    passed = jax.random.randint(jax.random.fold_in(own, 4), (count // 2,), 0, 1 << 20) % (room + 1)
    lengths = lengths.at[donor].add(-passed).at[receiver].add(passed)
    members = jnp.searchsorted(jnp.cumsum(lengths), jnp.arange(rows * top), side="right").astype(jnp.int32)
    table = members.reshape(top, rows).T
    table = table[jax.random.permutation(jax.random.fold_in(own, 1), rows)]
    offset_by = jax.random.randint(jax.random.fold_in(own, 2), (rows, 1), 0, top)
    return jnp.take_along_axis(table, (jnp.arange(top)[None, :] + offset_by) % top, axis=1)


def shares(number_of, total, most, skew, full):
    portions = [(1 << 20) // math.isqrt(grade ** skew) + 1 for grade in range(1, number_of + 1)]
    largest = most if full else min(most, max(-(-total // number_of), total * portions[0] // sum(portions)))
    least = 1 if total - largest >= number_of - 1 else 0
    counts, rest = [largest] + [least] * (number_of - 1), total - largest - least * (number_of - 1)
    while rest > 0:
        free = [i for i in range(1, number_of) if counts[i] < largest] or [i for i in range(1, number_of) if counts[i] < most]
        mass, budget = sum([portions[i] for i in free]), rest
        for i in free:
            extra = min(most - counts[i], max(1, budget * portions[i] // mass), rest)
            counts[i] = counts[i] + extra
            rest = rest - extra
    return np.array(counts)


def gaussian(stream_key, shape, spread, limit, cuts=(), kind=jnp.bfloat16):
    entries = spread * jax.random.normal(stream_key, shape, jnp.float32)
    if cuts:
        entries = entries * level_of(stream_key, shape, cuts, -0.22, 0.18)
    return jnp.clip(entries, -limit, limit).astype(kind)


def noise_with(key, extent, spread, bound, cuts, heavy, held_as=jnp.bfloat16):
    values = spread * jax.random.normal(key, extent, jnp.float32)
    if cuts:
        values = values * level_of(key, extent, cuts, -0.22, 0.18)
    return jnp.clip(spiked(values, jax.random.fold_in(key, 3), *heavy), -bound, bound).astype(held_as)


def setup_inputs(seed: int = 0) -> dict:
    arg_keys = jax.random.split(jax.random.key(seed), 15)
    moe_input = draw_moe_input(jax.random.fold_in(arg_keys[14], 71), 0)
    cotangent = noise_with(arg_keys[1], (TOKENS, D), 1.0, 6.0, ((0, 8),), (0, 1, 8, 2.0))
    routes_keys = jax.random.split(jax.random.fold_in(arg_keys[2], 1), TOKENS // TOK_DEV)
    routes_turns = jax.random.permutation(jax.random.fold_in(arg_keys[2], 3), TOKENS // TOK_DEV)
    routes = jax.vmap(lambda own, number: deal_out(jax.random.fold_in(arg_keys[2], 2), own, number, TOK_DEV, EXPERTS, TOP_K, CAP, 1))(routes_keys, routes_turns).reshape((TOKENS, TOP_K))
    route_weights = jnp.clip(0.2 + 0.8 * jax.random.uniform(arg_keys[3], (TOKENS, TOP_K), jnp.float32) ** level_of(arg_keys[3], (TOKENS, TOP_K), ((0, 8),), -0.2, 0.2), 0.2, 1.0)
    gate_weight = gaussian(arg_keys[4], (EXPERTS, D, FF), D ** -0.5, 0.125, ((0, 8), (2, 4)))
    up_weight = gaussian(arg_keys[5], (EXPERTS, D, FF), D ** -0.5, 0.125, ((0, 8), (2, 4)))
    down_weight = gaussian(arg_keys[6], (EXPERTS, FF, D), FF ** -0.5, 0.125, ((0, 8), (1, 4)))
    out_weight = gaussian(arg_keys[7], (D, HEADS * HEAD_DIM), D ** -0.5, 0.125, ((1, 4),))
    mixer_output = gaussian(arg_keys[8], (TOKENS, HEADS * HEAD_DIM), 1.0, 6.0, ((0, 8), (1, 4)))
    queries = gaussian(arg_keys[9], (TOKENS, HEADS * HEAD_DIM), 1.0, 6.0, ((0, 8), (1, 4)))
    key_vectors = gaussian(arg_keys[10], (TOKENS, HEADS * HEAD_DIM), HEAD_DIM ** -0.5, 0.75, ((0, 8), (1, 4)))
    value_vectors = gaussian(arg_keys[11], (TOKENS, HEADS * HEAD_DIM), 1.0, 6.0, ((0, 8), (1, 4)))
    log_decay = draw_log_decay(jax.random.fold_in(arg_keys[14], 71), 0)
    block_states = gaussian(arg_keys[13], (NBLK, HEADS, HEAD_DIM, HEAD_DIM), 0.25, 1.5, ((0, 8), (1, 4)))
    return {"moe_input": moe_input, "cotangent": cotangent, "routes": routes, "route_weights": route_weights, "gate_weight": gate_weight, "up_weight": up_weight, "down_weight": down_weight, "out_weight": out_weight, "mixer_output": mixer_output, "queries": queries, "key_vectors": key_vectors, "value_vectors": value_vectors, "log_decay": log_decay, "block_states": block_states}


clamp_limit = 7.0
sigmoid_sharpness = 1.702


def round_keep(values):
    return lax.optimization_barrier(values.astype(jnp.bfloat16)).astype(jnp.float32)


def pair_slots(routes_blocks):
    flat_routes = routes_blocks.reshape(routes_blocks.shape[0], -1)
    onehot = (flat_routes[:, :, None] == jnp.arange(EXPERTS, dtype=jnp.int32)[None, None, :]).astype(jnp.int32)
    before = jnp.cumsum(onehot, axis=1) - onehot
    return (flat_routes * CAP + jnp.sum(before * onehot, axis=2)).astype(jnp.int32)


def expert_grads(expert_rows, expert_cotangent, w_gate, w_up, w_down):
    gate_pre = jnp.dot(expert_rows, w_gate, preferred_element_type=jnp.float32)
    up_pre = jnp.dot(expert_rows, w_up, preferred_element_type=jnp.float32)
    act_grad = jnp.dot(expert_cotangent, w_down.T, preferred_element_type=jnp.float32)
    clamped = jnp.minimum(gate_pre, clamp_limit)
    logistic = jax.nn.sigmoid(sigmoid_sharpness * clamped)
    linear = jnp.clip(up_pre, -clamp_limit, clamp_limit)
    activation = (clamped * logistic * (linear + 1.0)).astype(jnp.bfloat16)
    slope_term = logistic + sigmoid_sharpness * clamped * logistic * (1.0 - logistic)
    gate_grad = jnp.where(gate_pre < clamp_limit, act_grad * (linear + 1.0) * slope_term, 0.0).astype(jnp.bfloat16)
    up_grad = jnp.where(jnp.abs(up_pre) < clamp_limit, act_grad * clamped * logistic, 0.0).astype(jnp.bfloat16)
    group_width = w_gate.shape[1] // N_TP
    gate_split = gate_grad.astype(jnp.float32).reshape(-1, N_TP, group_width)
    up_split = up_grad.astype(jnp.float32).reshape(-1, N_TP, group_width)
    partials = jnp.einsum("rgf,dgf->grd", gate_split, w_gate.astype(jnp.float32).reshape(-1, N_TP, group_width))
    partials = partials + jnp.einsum("rgf,dgf->grd", up_split, w_up.astype(jnp.float32).reshape(-1, N_TP, group_width))
    pair_grad = jnp.sum(round_keep(partials), axis=0).astype(jnp.bfloat16)
    grad_gate = jnp.dot(expert_rows.T, gate_grad, preferred_element_type=jnp.float32)
    grad_up = jnp.dot(expert_rows.T, up_grad, preferred_element_type=jnp.float32)
    grad_down = jnp.dot(activation.T, expert_cotangent, preferred_element_type=jnp.float32)
    return pair_grad, grad_gate, grad_up, grad_down


def retention_grads(queries, key_vectors, value_vectors, grad_mix, log_decay, block_states):
    blocks = TOKENS // BLK
    block_shape = (blocks, BLK, HEADS, HEAD_DIM)
    query_blocks = queries.astype(jnp.float32).reshape(block_shape)
    key_blocks = key_vectors.astype(jnp.float32).reshape(block_shape)
    value_blocks = value_vectors.astype(jnp.float32).reshape(block_shape)
    grad_blocks = grad_mix.astype(jnp.float32).reshape(block_shape)
    states = block_states.astype(jnp.float32)
    cumulative = jnp.cumsum(log_decay.reshape(blocks, BLK, HEADS), axis=1)
    block_ends = cumulative[:, -1, :]
    to_end = jnp.exp(block_ends[:, None, :] - cumulative)
    from_start = jnp.exp(cumulative)
    per_attention_head = jnp.transpose(cumulative, (0, 2, 1))
    differences = per_attention_head[:, :, :, None] - per_attention_head[:, :, None, :]
    causal = jnp.arange(BLK, dtype=jnp.int32)[:, None] >= jnp.arange(BLK, dtype=jnp.int32)[None, :]
    decays = jnp.where(causal, jnp.exp(jnp.minimum(differences, 0.0)), 0.0)
    weighted_grad = round_keep(jnp.einsum("nthe,nshe->nhts", grad_blocks, value_blocks) * decays)
    weighted_score = round_keep(jnp.einsum("nthd,nshd->nhts", query_blocks, key_blocks) * decays)
    query_intra = jnp.einsum("nhts,nshd->nthd", weighted_grad, key_blocks)
    query_carry = jnp.einsum("nthe,nhde->nthd", grad_blocks, states) * from_start[..., None]
    grad_queries = (query_intra + query_carry).astype(jnp.bfloat16).reshape(TOKENS, HEADS * HEAD_DIM)
    scaled_queries = round_keep(query_blocks * from_start[..., None])
    outer_terms = jnp.einsum("nthd,nthe->nhde", scaled_queries, grad_blocks)
    end_factor = jnp.exp(block_ends)

    def suffix_step(state_grad, inputs):
        factor, outer_block = inputs
        return factor[:, None, None] * state_grad + outer_block, state_grad

    start_grad = jnp.zeros((HEADS, HEAD_DIM, HEAD_DIM), jnp.float32)
    _, leaving = lax.scan(suffix_step, start_grad, (end_factor, outer_terms), reverse=True)
    carried = round_keep(leaving)
    key_intra = jnp.einsum("nhts,nthd->nshd", weighted_grad, query_blocks)
    value_intra = jnp.einsum("nhts,nthe->nshe", weighted_score, grad_blocks)
    key_carry = jnp.einsum("nshe,nhde->nshd", value_blocks, carried) * to_end[..., None]
    value_carry = jnp.einsum("nshd,nhde->nshe", key_blocks, carried) * to_end[..., None]
    grad_keys = (key_intra + key_carry).astype(jnp.bfloat16).reshape(TOKENS, HEADS * HEAD_DIM)
    grad_values = (value_intra + value_carry).astype(jnp.bfloat16).reshape(TOKENS, HEADS * HEAD_DIM)
    return grad_queries, grad_keys, grad_values


def reference(moe_input, cotangent, routes, route_weights, gate_weight, up_weight, down_weight, out_weight, mixer_output, queries, key_vectors, value_vectors, log_decay, block_states):
    pair_count = TOK_DEV * TOP_K
    slot_index = pair_slots(routes.reshape(N_SP, TOK_DEV, TOP_K))
    source = jnp.arange(N_SP, dtype=jnp.int32)[:, None]
    pair_ids = (source * pair_count + jnp.arange(pair_count, dtype=jnp.int32)[None, :]).astype(jnp.int32)
    slot_pair = jnp.full((N_SP, EXPERTS * CAP), TOKENS * TOP_K, jnp.int32).at[source, slot_index].set(pair_ids)
    tables = jnp.transpose(slot_pair.reshape(N_SP, EXPERTS, CAP), (1, 0, 2)).reshape(EXPERTS, N_SP * CAP)
    zero_row = jnp.zeros((1, D), jnp.bfloat16)
    scaled = (route_weights[:, :, None] * cotangent.astype(jnp.float32)[:, None, :]).astype(jnp.bfloat16)
    scaled = jnp.concatenate([scaled.reshape(TOKENS * TOP_K, D), zero_row], axis=0)
    inputs_padded = jnp.concatenate([moe_input, zero_row], axis=0)

    def one_expert(operands):
        table, w_gate, w_up, w_down = operands
        return expert_grads(inputs_padded[table // TOP_K], scaled[table], w_gate, w_up, w_down)

    pair_rows, grad_gate, grad_up, grad_down = lax.map(one_expert, (tables, gate_weight, up_weight, down_weight))
    pair_sum = jnp.zeros((TOKENS * TOP_K + 1, D), jnp.float32).at[tables.reshape(-1)].add(pair_rows.reshape(-1, D).astype(jnp.float32))
    token_sum = jnp.sum(pair_sum[:TOKENS * TOP_K].reshape(TOKENS, TOP_K, D), axis=1)
    residual_grad = (cotangent.astype(jnp.float32) + token_sum).astype(jnp.bfloat16)
    grad_out = jnp.dot(residual_grad.T, mixer_output, preferred_element_type=jnp.float32)
    grad_mix = jnp.dot(residual_grad, out_weight, preferred_element_type=jnp.float32).astype(jnp.bfloat16)
    grad_queries, grad_keys, grad_values = retention_grads(queries, key_vectors, value_vectors, grad_mix, log_decay, block_states)
    return (grad_gate, grad_up, grad_down, grad_out, grad_queries, grad_keys, grad_values)
```

```python
import functools

import jax
import jax.numpy as jnp
from jax import lax
from jax.experimental import pallas as pl
from jax.experimental.pallas import tpu as pltpu
from jax.sharding import PartitionSpec as P

TOP_K = 2

clamp_limit = 7.0
sigmoid_sharpness = 1.702
BF = jnp.bfloat16
F32 = jnp.float32


def contract(left, right, l_dim, r_dim, precision=None):
    return lax.dot_general(
        left,
        right,
        (((l_dim,), (r_dim,)), ((), ())),
        preferred_element_type=F32,
        precision=precision,
    )


def exact(left, right):
    return contract(left, right, 1, 0, precision=lax.Precision.HIGHEST)


def kernel_call(body, outs, args, flops, name, scalars=None, in_specs=None, scratch=(), anys=0):
    out_shape = [jax.ShapeDtypeStruct(shape, dtype) for shape, dtype in outs]
    moved = sum(a.size * a.dtype.itemsize for a in args)
    moved += sum(o.size * o.dtype.itemsize for o in out_shape)
    cost = pl.CostEstimate(flops=int(flops), bytes_accessed=int(moved), transcendentals=0)
    params = pltpu.CompilerParams(vmem_limit_bytes=58 * 1024 * 1024)
    space = pl.ANY if anys else pltpu.VMEM
    if scalars is None:
        return pl.pallas_call(
            body,
            out_shape=out_shape,
            in_specs=[pl.BlockSpec(memory_space=pltpu.VMEM)] * len(args),
            out_specs=[pl.BlockSpec(memory_space=space)] * len(outs),
            scratch_shapes=list(scratch),
            compiler_params=params,
            cost_estimate=cost,
            name=name,
        )(*args)
    grid_spec = pltpu.PrefetchScalarGridSpec(
        num_scalar_prefetch=1,
        grid=(1,),
        in_specs=in_specs,
        out_specs=[
            pl.BlockSpec(shape, functools.partial(lambda n, i, sc: (0,) * n, len(shape)))
            for shape, _ in outs
        ],
        scratch_shapes=list(scratch),
    )
    return pl.pallas_call(
        body,
        grid_spec=grid_spec,
        out_shape=out_shape,
        compiler_params=params,
        cost_estimate=cost,
        name=name,
    )(scalars, *args)


def whole(array):
    return pl.BlockSpec(array.shape, functools.partial(lambda n, i, sc: (0,) * n, array.ndim))


def dispatch_body(n, cap, sc, x, cot, routes, weights, *outs):
    place = sc[0]
    tokens = x.shape[0]
    rel = routes[...] ^ place
    rel0, rel1 = rel[0:1, :], rel[1:2, :]
    expert = lax.broadcasted_iota(jnp.int32, (n, tokens), 0)
    hit0, hit1 = expert == rel0, expert == rel1
    both = (hit0 | hit1).astype(F32).astype(BF)
    earlier = lax.broadcasted_iota(jnp.int32, (tokens, tokens), 0) < lax.broadcasted_iota(
        jnp.int32, (tokens, tokens), 1
    )
    before = contract(both, earlier.astype(F32).astype(BF), 1, 0)
    slot0 = rel0 * cap + jnp.sum(jnp.where(hit0, before, 0.0), axis=0, keepdims=True).astype(
        jnp.int32
    )
    slot1 = rel1 * cap + jnp.sum(jnp.where(hit1, before, 0.0), axis=0, keepdims=True).astype(
        jnp.int32
    )
    rows = lax.broadcasted_iota(jnp.int32, (n * cap, tokens), 0)
    pick0 = (rows == slot0).astype(F32).astype(BF)
    pick1 = (rows == slot1).astype(F32).astype(BF)
    pick = pick0 + pick1
    outs[2 * n][...] = pick
    sent = contract(pick, x[...], 1, 0).astype(BF)
    cot32 = cot[...].astype(F32)
    w = weights[...]
    scaled0 = (w[:, 0:1] * cot32).astype(BF)
    scaled1 = (w[:, 1:2] * cot32).astype(BF)
    grads = (contract(pick0, scaled0, 1, 0) + contract(pick1, scaled1, 1, 0)).astype(BF)
    for k in range(n):
        outs[k][...] = sent[k * cap : (k + 1) * cap]
        outs[n + k][...] = grads[k * cap : (k + 1) * cap]


def pre_body(gate_rows, *refs):
    xs, w_gate, w_up, gate_pre, up_pre = refs[:4], refs[4], refs[5], refs[6], refs[7]
    del gate_rows
    place = lax.axis_index("tp")
    for w, out in ((w_gate, gate_pre), (w_up, up_pre)):
        total = None
        for m in range(4):
            at = pl.multiple_of((place ^ m) * xs[m].shape[1], xs[m].shape[1])
            term = contract(xs[m][...], w[0, pl.ds(at, xs[m].shape[1]), :], 1, 0)
            total = term if total is None else total + term
        out[...] = total


def expert_body(*refs):
    ys, (w_gate, w_up, w_down, gate_pre, up_pre) = refs[:4], refs[4:9]
    gate_grad_out, up_grad_out, act_out, near, far0, far1 = refs[9:15]
    share = ys[0].shape[1]
    place = lax.axis_index("tp")
    act_grad = None
    for m in range(4):
        at = pl.multiple_of((place ^ m) * share, share)
        term = contract(ys[m][...], w_down[0, :, pl.ds(at, share)], 1, 1)
        act_grad = term if act_grad is None else act_grad + term
    gate, up = gate_pre[...], up_pre[...]
    clamped = jnp.minimum(gate, clamp_limit)
    logistic = jax.nn.sigmoid(sigmoid_sharpness * clamped)
    linear = jnp.clip(up, -clamp_limit, clamp_limit)
    gated = clamped * logistic
    act_out[...] = (gated * (linear + 1.0)).astype(BF)
    slope = logistic + sigmoid_sharpness * gated * (1.0 - logistic)
    gate_grad = jnp.where(gate < clamp_limit, act_grad * (linear + 1.0) * slope, 0.0).astype(BF)
    up_grad = jnp.where(jnp.abs(up) < clamp_limit, act_grad * gated, 0.0).astype(BF)
    gate_grad_out[...] = gate_grad
    up_grad_out[...] = up_grad
    for m in (3, 1, 2, 0):
        at = pl.multiple_of((place ^ m) * share, share)
        term = contract(gate_grad, w_gate[0, pl.ds(at, share), :], 1, 1)
        term = (term + contract(up_grad, w_up[0, pl.ds(at, share), :], 1, 1)).astype(BF)
        if m == 3:
            near[0] = term
        elif m == 1:
            near[1] = term
        elif m == 2:
            far0[...] = term
        else:
            far1[...] = term


def weight_grad_body(groups, *refs):
    xs = [refs[4 * g : 4 * g + 4] for g in range(groups)]
    ys = [refs[4 * groups + 4 * g : 4 * groups + 4 * g + 4] for g in range(groups)]
    rest = refs[8 * groups :]
    gate_grads, up_grads, acts = rest[:groups], rest[groups : 2 * groups], rest[2 * groups : 3 * groups]
    out_gate, out_up, out_down, hold, sems = rest[3 * groups :]
    place = lax.axis_index("tp")
    share = xs[0][0].shape[1]
    copies = []
    for m in range(4):
        at = pl.multiple_of((place ^ m) * share, share)
        x = jnp.concatenate([xs[g][m][...] for g in range(groups)], axis=0)
        y = jnp.concatenate([ys[g][m][...] for g in range(groups)], axis=0)
        for i, (lefts, right) in enumerate((((x,), gate_grads), ((x,), up_grads), (acts, (y,)))):
            if i < 2:
                value = contract(x, jnp.concatenate([r[...] for r in right], axis=0), 0, 0)
                dst = (out_gate, out_up)[i].at[0, pl.ds(at, share), :]
            else:
                value = contract(jnp.concatenate([r[...] for r in lefts], axis=0), y, 0, 0)
                dst = out_down.at[0, :, pl.ds(at, share)]
            hold[3 * m + i] = value
            copy = pltpu.make_async_copy(hold.at[3 * m + i], dst, sems.at[3 * m + i])
            copy.start()
            copies.append(copy)
    for copy in copies:
        copy.wait()


def near_sum_body(far0, near0, out):
    out[...] = (far0[...].astype(F32) + near0[...].astype(F32)).astype(BF)


def far_sum_body(cap, count, own, near, got, *outs):
    total = (own[...].astype(F32) + near[1].astype(F32) + got[...].astype(F32)).astype(BF)
    for i in range(count):
        outs[i][...] = total[i * cap : (i + 1) * cap]


def combine_body(n, cap, sc, cot, pick, *refs):
    returned, out = refs[:n], refs[n]
    if cap % 16 == 0:
        rows = jnp.concatenate([r[...] for r in returned], axis=0)
        total = contract(pick[...], rows, 0, 0)
    else:
        total = None
        for k in range(n):
            term = contract(pick[k * cap : (k + 1) * cap, :], returned[k][...], 0, 0)
            total = term if total is None else total + term
    out[...] = (cot[...].astype(F32) + total).astype(BF)


def retention_pre_body(blocks, log_decay, log_decay_t, q, k, decays, scores, scaled, start, end, ends):
    rows = q.shape[0] // blocks
    heads = log_decay.shape[1]
    width = q.shape[1]
    dim = width // heads
    t = lax.broadcasted_iota(jnp.int32, (rows, rows), 0)
    s = lax.broadcasted_iota(jnp.int32, (rows, rows), 1)
    causal = s <= t
    lower = causal.astype(F32)
    upper = (t <= s).astype(F32)
    spread = (
        lax.broadcasted_iota(jnp.int32, (heads, width), 0)
        == lax.broadcasted_iota(jnp.int32, (heads, width), 1) // dim
    ).astype(F32)
    lane = lax.broadcasted_iota(jnp.int32, (rows, 2 * dim), 1)
    for b in range(blocks):
        at = slice(b * rows, (b + 1) * rows)
        cum = exact(lower, log_decay[at, :])
        cum_t = exact(log_decay_t[:, at], upper)
        wide = exact(cum, spread)
        from_start = jnp.exp(wide)
        last = wide[rows - 1 : rows, :]
        start[at, :] = from_start
        end[at, :] = jnp.exp(last - wide)
        ends[b : b + 1, :] = jnp.exp(last)
        scaled[at, :] = (q[at, :].astype(F32) * from_start).astype(BF)
        for h in range(heads):
            pair = slice(h // 2 * 2 * dim, (h // 2 + 1) * 2 * dim)
            decay = jnp.where(
                causal, jnp.exp(jnp.minimum(cum[:, h : h + 1] - cum_t[h : h + 1, :], 0.0)), 0.0
            )
            decays[b, h] = decay
            own = jnp.where(lane // dim == h % 2, q[at, pair], jnp.zeros((), BF))
            scores[b, h] = (contract(own, k[at, pair], 1, 1) * decay).astype(BF)


def mix_body(blocks, heads, *refs):
    pieces = refs[:4]
    w_out, scaled, ends, grad_mix, message, later = refs[4:]
    place = lax.axis_index("tp")
    share = pieces[0].shape[1]
    total = None
    for m in range(4):
        at = pl.multiple_of((place ^ m) * share, share)
        term = contract(pieces[m][...], w_out[pl.ds(at, share), :], 1, 0)
        total = term if total is None else total + term
    grad = total.astype(BF)
    grad_mix[...] = grad
    rows = grad.shape[0] // blocks
    width = grad.shape[1]
    dim = width // heads
    lane = lax.broadcasted_iota(jnp.int32, (dim, 2 * dim), 1)
    running = None
    for b in reversed(range(blocks)):
        parts = []
        for p in range(heads // 2):
            at, pair = slice(b * rows, (b + 1) * rows), slice(p * 2 * dim, (p + 1) * 2 * dim)
            full = contract(scaled[at, pair], grad[at, pair], 0, 0)
            parts.append(jnp.where(lane < dim, full[:dim], full[dim:]))
        outer = jnp.concatenate(parts, axis=1)
        if b > 0:
            later[b - 1] = outer
        running = outer if running is None else ends[b : b + 1, :] * running + outer
    message[:dim, :] = running.astype(BF)
    factor = ends[0:1, :]
    for b in range(1, blocks):
        factor = factor * ends[b : b + 1, :]
    message[dim:, :] = jnp.broadcast_to(factor, (8, width)).astype(BF)


def paired(square, dim):
    both = jnp.concatenate([square, square], axis=0)
    row = lax.broadcasted_iota(jnp.int32, both.shape, 0)
    lane = lax.broadcasted_iota(jnp.int32, both.shape, 1)
    return jnp.where((row < dim) == (lane < dim), both, jnp.zeros((), both.dtype))


def local_body(blocks, heads, grad, q, k, v, decays, scores, start, states, out_q, key_in, value_in):
    rows = q.shape[0] // blocks
    dim = q.shape[1] // heads
    lane = lax.broadcasted_iota(jnp.int32, (rows, 2 * dim), 1)
    zero = jnp.zeros((), BF)
    for b in range(blocks):
        for p in range(heads // 2):
            at, pair = slice(b * rows, (b + 1) * rows), slice(p * 2 * dim, (p + 1) * 2 * dim)
            g, qq, kk, vv = grad[at, pair], q[at, pair], k[at, pair], v[at, pair]
            carry = contract(g, paired(states[b, :, pair], dim), 1, 1)
            to_q = carry * start[at, pair]
            to_k = to_v = None
            for i in range(2):
                mine = lane // dim == i
                g_own = jnp.where(mine, g, zero)
                weighted = (contract(g_own, vv, 1, 1) * decays[b, 2 * p + i]).astype(BF)
                to_q = to_q + contract(weighted, jnp.where(mine, kk, zero), 1, 0)
                a = contract(weighted, jnp.where(mine, qq, zero), 0, 0)
                c = contract(scores[b, 2 * p + i], g_own, 0, 0)
                to_k = a if to_k is None else to_k + a
                to_v = c if to_v is None else to_v + c
            out_q[at, pair] = to_q.astype(BF)
            key_in[at, pair] = to_k
            value_in[at, pair] = to_v


def carry_body(n, blocks, heads, *refs):
    messages = refs[:n]
    k, v, key_in, value_in, end, ends, later, out_k, out_v, factors, weights = refs[n:]
    place = lax.axis_index("sp")
    rows = k.shape[0] // blocks
    width = k.shape[1]
    dim = width // heads
    for j in range(n):
        factors[pl.ds(place ^ j, 1), :] = messages[j][dim : dim + 1, :].astype(F32)
    running = jnp.ones((1, width), F32)
    for u in range(n):
        ahead = u > place
        weights[pl.ds(place ^ u, 1), :] = jnp.where(ahead, running, 0.0)
        running = jnp.where(ahead, running * factors[u : u + 1, :], running)
    state = jnp.zeros((dim, width), F32)
    for j in range(1, n):
        state = state + weights[j : j + 1, :] * messages[j][:dim, :].astype(F32)
    for b in reversed(range(blocks)):
        carried = state.astype(BF)
        if b > 0:
            state = ends[b : b + 1, :] * state + later[b - 1]
        for p in range(heads // 2):
            at, pair = slice(b * rows, (b + 1) * rows), slice(p * 2 * dim, (p + 1) * 2 * dim)
            square = paired(carried[:, pair], dim)
            scale = end[at, pair]
            out_k[at, pair] = (
                key_in[at, pair] + contract(v[at, pair], square, 1, 1) * scale
            ).astype(BF)
            out_v[at, pair] = (
                value_in[at, pair] + contract(k[at, pair], square, 1, 0) * scale
            ).astype(BF)


def split_body(n, *refs):
    pieces, outs, full = refs[:4], refs[4 : 4 + n], refs[4 + n]
    tp, sp = lax.axis_index("tp"), lax.axis_index("sp")
    share = pieces[0].shape[1]
    half = full.shape[0]
    top = pl.multiple_of((tp & 1) * half, half)
    for m in range(4):
        at = pl.multiple_of((tp ^ m) * share, share)
        full[:, pl.ds(at, share)] = pieces[m][pl.ds(top, half), :]
    width = outs[0].shape[1]
    for k in range(n):
        at = pl.multiple_of((sp ^ k) * width, width)
        outs[k][...] = full[:, pl.ds(at, width)]


def out_grad_body(n, own, other, *refs):
    mixers, out = refs[:n], refs[n]
    half = own.shape[0] // n
    top = pl.multiple_of((lax.axis_index("tp") & 1) * half, half)
    low = pl.multiple_of((1 - (lax.axis_index("tp") & 1)) * half, half)
    total = None
    for k in range(n):
        at = slice(k * half, (k + 1) * half)
        term = contract(own[at, :], mixers[k][pl.ds(top, half), :], 0, 0)
        term = term + contract(other[at, :], mixers[k][pl.ds(low, half), :], 0, 0)
        total = term if total is None else total + term
    out[...] = total


def shards(
    moe_input,
    cotangent,
    routes,
    route_weights,
    gate_weight,
    up_weight,
    down_weight,
    out_weight,
    mixer_output,
    queries,
    key_vectors,
    value_vectors,
    log_decay,
    block_states,
):
    tokens, width = cotangent.shape
    n = lax.axis_size("sp")
    cap = 5 * tokens * TOP_K // (4 * n)
    share = width // lax.axis_size("tp")
    hidden = gate_weight.shape[2]
    sp, tp = lax.axis_index("sp"), lax.axis_index("tp")
    places = jnp.stack([sp, tp]).astype(jnp.int32)
    groups = [list(range(n // 2, n)), list(range(n // 2))]

    def over_sp(x, k):
        if k == 0:
            return x
        return lax.ppermute(x, "sp", [(i, i ^ k) for i in range(n)])

    def over_tp(x, m):
        return lax.ppermute(x, "tp", [(i, i ^ m) for i in range(4)])

    def spread_tp(x):
        across = over_tp(x, 2)
        return [x, over_tp(x, 1), across, over_tp(across, 1)]

    share_spec = pl.BlockSpec((tokens, share), lambda i, sc: (0, sc[1]))
    routes_t = routes.T
    outs = kernel_call(
        functools.partial(dispatch_body, n, cap),
        [((cap, share), BF)] * (2 * n) + [((n * cap, tokens), BF)],
        (moe_input, cotangent, routes_t, route_weights),
        6 * n * cap * tokens * share,
        "dispatch",
        scalars=places,
        in_specs=[share_spec, share_spec, whole(routes_t), whole(route_weights)],
    )
    pick = outs[2 * n]

    order = [k for group in groups for k in group]
    x_in = {k: over_sp(outs[k], k) for k in order}
    y_in = {k: over_sp(outs[n + k], k) for k in order}
    xs = [spread_tp(jnp.concatenate([x_in[k] for k in group], axis=0)) for group in groups]
    ys = [spread_tp(jnp.concatenate([y_in[k] for k in group], axis=0)) for group in groups]

    heads = log_decay.shape[1]
    blocks = block_states.shape[0]
    dim = queries.shape[1] // heads
    rows = tokens // blocks
    local = queries.shape[1]
    decays, scores, scaled, start, end, ends = kernel_call(
        functools.partial(retention_pre_body, blocks),
        [
            ((blocks, heads, rows, rows), F32),
            ((blocks, heads, rows, rows), BF),
            ((tokens, local), BF),
            ((tokens, local), F32),
            ((tokens, local), F32),
            ((blocks, local), F32),
        ],
        (log_decay, log_decay.T, queries, key_vectors),
        10 * tokens * rows * local,
        "retention_pre",
    )
    states = block_states.transpose(0, 2, 1, 3).reshape(blocks, dim, heads * dim)

    mixer_held, _ = lax.optimization_barrier((mixer_output, y_in[n - 1]))
    mixers = [over_sp(mixer_held, k) for k in range(n)]

    pres = []
    for g in range(len(groups)):
        count = xs[g][0].shape[0]
        pres.append(
            kernel_call(
                functools.partial(pre_body, g),
                [((count, hidden), F32)] * 2,
                (*xs[g], gate_weight, up_weight),
                4 * count * width * hidden,
                "gate_up",
            )
        )
    gate_grads, up_grads, acts, returned = [], [], [], {}
    for g, group in enumerate(groups):
        count = xs[g][0].shape[0]
        gate_grad, up_grad, act, near, far0, far1 = kernel_call(
            expert_body,
            [((count, hidden), BF)] * 3
            + [((2, count, share), BF), ((count, share), BF), ((count, share), BF)],
            (*ys[g], gate_weight, up_weight, down_weight, *pres[g]),
            6 * count * width * hidden,
            "expert",
        )
        gate_grads.append(gate_grad)
        up_grads.append(up_grad)
        acts.append(act)
        near_in = over_tp(near, 1)
        (send,) = kernel_call(
            near_sum_body,
            [((count, share), BF)],
            (far0, near_in[0]),
            count * share,
            "near_sum",
        )
        got = over_tp(send, 2)
        back = kernel_call(
            functools.partial(far_sum_body, cap, len(group)),
            [((cap, share), BF)] * len(group),
            (far1, near_in, got),
            3 * count * share,
            "far_sum",
        )
        for k, piece in zip(group, back):
            returned[k] = over_sp(piece, k)

    flat = [x for xg in xs for x in xg] + [y for yg in ys for y in yg]
    grad_gate, grad_up, grad_down = kernel_call(
        functools.partial(weight_grad_body, len(groups)),
        [((1, width, hidden), F32), ((1, width, hidden), F32), ((1, hidden, width), F32)],
        (*flat, *gate_grads, *up_grads, *acts),
        6 * n * cap * width * hidden,
        "weight_grads",
        scratch=[pltpu.VMEM((12, share, hidden), F32), pltpu.SemaphoreType.DMA((12,))],
        anys=1,
    )

    back_rows = [returned[k] for k in range(n)]
    (residual,) = kernel_call(
        functools.partial(combine_body, n, cap),
        [((tokens, share), BF)],
        (cotangent, pick, *back_rows),
        2 * n * cap * tokens * share,
        "combine",
        scalars=places,
        in_specs=[share_spec, whole(pick)] + [whole(r) for r in back_rows],
    )
    pieces = spread_tp(residual)
    grad_mix, message, later = kernel_call(
        functools.partial(mix_body, blocks, heads),
        [((tokens, local), BF), ((dim + 8, local), BF), ((blocks - 1, dim, local), F32)],
        (*pieces, out_weight, scaled, ends),
        2 * tokens * width * local,
        "mix",
    )
    messages = [over_sp(message, k) for k in range(n)]

    block = width // n
    half = tokens // 2
    if block % 128 == 0:
        split = kernel_call(
            functools.partial(split_body, n),
            [((half, block), BF)] * n,
            pieces,
            tokens * width,
            "split",
            scratch=[pltpu.VMEM((half, width), BF)],
        )
    else:
        ordered = jnp.concatenate(pieces, axis=1).reshape(tokens, 4, share)
        ordered = jnp.take(ordered, tp ^ jnp.arange(4), axis=1).reshape(tokens, width)
        mine = lax.dynamic_slice_in_dim(ordered, (tp & 1) * half, half, 0)
        split = [
            lax.dynamic_slice_in_dim(mine, (sp ^ k) * block, block, 1) for k in range(n)
        ]
    own = jnp.concatenate([over_sp(split[k], k) for k in range(n)], axis=0)
    other = over_tp(own, 1)

    grad_queries, key_in, value_in = kernel_call(
        functools.partial(local_body, blocks, heads),
        [((tokens, local), BF), ((tokens, local), F32), ((tokens, local), F32)],
        (grad_mix, queries, key_vectors, value_vectors, decays, scores, start, states),
        20 * tokens * rows * local,
        "local",
    )
    grad_keys, grad_values = kernel_call(
        functools.partial(carry_body, n, blocks, heads),
        [((tokens, local), BF)] * 2,
        (*messages, key_vectors, value_vectors, key_in, value_in, end, ends, later),
        8 * tokens * dim * local,
        "carry",
        scratch=[pltpu.VMEM((n, local), F32), pltpu.VMEM((n, local), F32)],
    )
    (grad_out,) = kernel_call(
        functools.partial(out_grad_body, n),
        [((block, mixer_output.shape[1]), F32)],
        (own, other, *mixers),
        2 * n * tokens * block * mixer_output.shape[1],
        "out_grad",
    )
    return (grad_gate, grad_up, grad_down, grad_out, grad_queries, grad_keys, grad_values)


def solution(mesh):
    return jax.shard_map(
        shards,
        mesh=mesh,
        in_specs=(
            P("sp", None),
            P("sp", None),
            P("sp", None),
            P("sp", None),
            P("sp", None, "tp"),
            P("sp", None, "tp"),
            P("sp", "tp", None),
            P(None, "tp"),
            P("sp", "tp"),
            P("sp", "tp"),
            P("sp", "tp"),
            P("sp", "tp"),
            P("sp", "tp"),
            P("sp", "tp", None, None),
        ),
        out_specs=(
            P("sp", None, "tp"),
            P("sp", None, "tp"),
            P("sp", "tp", None),
            P("sp", "tp"),
            P("sp", "tp"),
            P("sp", "tp"),
            P("sp", "tp"),
        ),
        check_vma=False,
    )
```

```python
import functools

import jax
import jax.numpy as jnp
from jax import lax
from jax.experimental import pallas as pl
from jax.experimental.pallas import tpu as pltpu
from jax.sharding import PartitionSpec as P


TOP_K = 2

clamp_limit = 7.0
sigmoid_sharpness = 1.702
BF = jnp.bfloat16
F32 = jnp.float32


def contract(left, right, l_dim, r_dim, precision=None):
    return lax.dot_general(
        left,
        right,
        (((l_dim,), (r_dim,)), ((), ())),
        preferred_element_type=F32,
        precision=precision,
    )


def exact(left, right):
    return contract(left, right, 1, 0, precision=lax.Precision.HIGHEST)


def kernel_call(body, outs, args, flops, scratch=(), vmem=8, far=(), far_out=False):
    out_shape = [jax.ShapeDtypeStruct(shape, dtype) for shape, dtype in outs]
    moved = sum(a.size * a.dtype.itemsize for a in args)
    moved += sum(o.size * o.dtype.itemsize for o in out_shape)
    return pl.pallas_call(
        body,
        out_shape=out_shape,
        in_specs=[
            pl.BlockSpec(memory_space=pl.ANY if i in far else pltpu.VMEM)
            for i in range(len(args))
        ],
        out_specs=[pl.BlockSpec(memory_space=pl.ANY if far_out else pltpu.VMEM)] * len(outs),
        scratch_shapes=list(scratch),
        compiler_params=pltpu.CompilerParams(vmem_limit_bytes=vmem * 1024 * 1024),
        cost_estimate=pl.CostEstimate(
            flops=int(flops), bytes_accessed=int(moved), transcendentals=0
        ),
    )(*args)


def dispatch_body(n, cap, x_all, cot_all, routes, weights, *refs):
    outs, (x, cot, sems) = refs[: 2 * n + 1], refs[2 * n + 1 :]
    tokens, share = x.shape
    at = pl.multiple_of(lax.axis_index("tp") * share, share)
    copies = [
        pltpu.make_async_copy(src.at[:, pl.ds(at, share)], dst, sems.at[i])
        for i, (src, dst) in enumerate(((x_all, x), (cot_all, cot)))
    ]
    for copy in copies:
        copy.start()
    rel = routes[...] ^ lax.axis_index("sp")
    rel0, rel1 = rel[0:1, :], rel[1:2, :]
    expert = lax.broadcasted_iota(jnp.int32, (n, tokens), 0)
    hit0, hit1 = expert == rel0, expert == rel1
    both = (hit0 | hit1).astype(F32).astype(BF)
    earlier = lax.broadcasted_iota(jnp.int32, (tokens, tokens), 0) < lax.broadcasted_iota(
        jnp.int32, (tokens, tokens), 1
    )
    before = contract(both, earlier.astype(F32).astype(BF), 1, 0)
    slot0 = rel0 * cap + jnp.sum(jnp.where(hit0, before, 0.0), axis=0, keepdims=True).astype(
        jnp.int32
    )
    slot1 = rel1 * cap + jnp.sum(jnp.where(hit1, before, 0.0), axis=0, keepdims=True).astype(
        jnp.int32
    )
    rows = lax.broadcasted_iota(jnp.int32, (n * cap, tokens), 0)
    pick0, pick1 = rows == slot0, rows == slot1
    w = weights[...]
    scale = jnp.where(pick0, w[0:1, :], jnp.where(pick1, w[1:2, :], 0.0))
    scale = jnp.sum(scale, axis=1, keepdims=True)
    pick = (pick0 | pick1).astype(F32).astype(BF)
    outs[2 * n][...] = pick
    copies[0].wait()
    sent = contract(pick, x[...], 1, 0).astype(BF)
    for k in range(n):
        outs[k][...] = sent[k * cap : (k + 1) * cap]
    copies[1].wait()
    grads = (contract(pick, cot[...], 1, 0) * scale).astype(BF)
    for k in range(n):
        outs[n + k][...] = grads[k * cap : (k + 1) * cap]


def pre_body(gate_rows, *refs):
    xs, w_gate, w_up, gate_pre, up_pre = refs[:4], refs[4], refs[5], refs[6], refs[7]
    del gate_rows
    place = lax.axis_index("tp")
    for w, out in ((w_gate, gate_pre), (w_up, up_pre)):
        total = None
        for m in range(4):
            at = pl.multiple_of((place ^ m) * xs[m].shape[1], xs[m].shape[1])
            term = contract(xs[m][...], w[0, pl.ds(at, xs[m].shape[1]), :], 1, 0)
            total = term if total is None else total + term
        out[...] = total


def expert_body(*refs):
    ys, (w_gate, w_up, w_down, gate_pre, up_pre) = refs[:4], refs[4:9]
    gate_grad_out, up_grad_out, act_out, near, far0, far1 = refs[9:15]
    share = ys[0].shape[1]
    place = lax.axis_index("tp")
    act_grad = None
    for m in range(4):
        at = pl.multiple_of((place ^ m) * share, share)
        term = contract(ys[m][...], w_down[0, :, pl.ds(at, share)], 1, 1)
        act_grad = term if act_grad is None else act_grad + term
    gate, up = gate_pre[...], up_pre[...]
    clamped = jnp.minimum(gate, clamp_limit)
    logistic = jax.nn.sigmoid(sigmoid_sharpness * clamped)
    linear = jnp.clip(up, -clamp_limit, clamp_limit)
    gated = clamped * logistic
    act_out[...] = (gated * (linear + 1.0)).astype(BF)
    slope = logistic + sigmoid_sharpness * gated * (1.0 - logistic)
    gate_grad = jnp.where(gate < clamp_limit, act_grad * (linear + 1.0) * slope, 0.0).astype(BF)
    up_grad = jnp.where(jnp.abs(up) < clamp_limit, act_grad * gated, 0.0).astype(BF)
    gate_grad_out[...] = gate_grad
    up_grad_out[...] = up_grad
    for m in (3, 1, 2, 0):
        at = pl.multiple_of((place ^ m) * share, share)
        term = contract(gate_grad, w_gate[0, pl.ds(at, share), :], 1, 1)
        term = (term + contract(up_grad, w_up[0, pl.ds(at, share), :], 1, 1)).astype(BF)
        if m == 3:
            near[0] = term
        elif m == 1:
            near[1] = term
        elif m == 2:
            far0[...] = term
        else:
            far1[...] = term


def weight_grad_body(groups, *refs):
    xs = [refs[4 * g : 4 * g + 4] for g in range(groups)]
    ys = [refs[4 * groups + 4 * g : 4 * groups + 4 * g + 4] for g in range(groups)]
    rest = refs[8 * groups :]
    gate_grads, up_grads, acts = rest[:groups], rest[groups : 2 * groups], rest[2 * groups : 3 * groups]
    out_gate, out_up, out_down, hold, sems = rest[3 * groups :]
    place = lax.axis_index("tp")
    share = xs[0][0].shape[1]
    copies = []
    for m in range(4):
        at = pl.multiple_of((place ^ m) * share, share)
        x = jnp.concatenate([xs[g][m][...] for g in range(groups)], axis=0)
        y = jnp.concatenate([ys[g][m][...] for g in range(groups)], axis=0)
        for i, (lefts, right) in enumerate((((x,), gate_grads), ((x,), up_grads), (acts, (y,)))):
            if i < 2:
                value = contract(x, jnp.concatenate([r[...] for r in right], axis=0), 0, 0)
                dst = (out_gate, out_up)[i].at[0, pl.ds(at, share), :]
            else:
                value = contract(jnp.concatenate([r[...] for r in lefts], axis=0), y, 0, 0)
                dst = out_down.at[0, :, pl.ds(at, share)]
            hold[3 * m + i] = value
            copy = pltpu.make_async_copy(hold.at[3 * m + i], dst, sems.at[3 * m + i])
            copy.start()
            copies.append(copy)
    for copy in copies:
        copy.wait()


def near_sum_body(far0, near, out):
    out[...] = (far0[...].astype(F32) + near[0].astype(F32)).astype(BF)


def far_sum_body(cap, count, own, near, got, *outs):
    total = (own[...].astype(F32) + near[1].astype(F32) + got[...].astype(F32)).astype(BF)
    for i in range(count):
        outs[i][...] = total[i * cap : (i + 1) * cap]


def combine_body(n, cap, cot_all, pick_t, *refs):
    returned, (out, cot, sem) = refs[:n], refs[n:]
    share = cot.shape[1]
    at = pl.multiple_of(lax.axis_index("tp") * share, share)
    copy = pltpu.make_async_copy(cot_all.at[:, pl.ds(at, share)], cot, sem.at[0])
    copy.start()
    if cap % 16 == 0:
        rows = jnp.concatenate([r[...] for r in returned], axis=0)
        total = contract(pick_t[...], rows, 1, 0)
    else:
        picked = pick_t[...]
        total = None
        for k in range(n):
            term = contract(picked[:, k * cap : (k + 1) * cap], returned[k][...], 1, 0)
            total = term if total is None else total + term
    copy.wait()
    out[...] = (cot[...].astype(F32) + total).astype(BF)


def retention_pre_body(blocks, log_decay, log_decay_t, q, k, decays, scores, scaled, start, end, ends):
    rows = q.shape[0] // blocks
    heads = log_decay.shape[1]
    width = q.shape[1]
    dim = width // heads
    t = lax.broadcasted_iota(jnp.int32, (rows, rows), 0)
    s = lax.broadcasted_iota(jnp.int32, (rows, rows), 1)
    causal = s <= t
    lower = causal.astype(F32)
    upper = (t <= s).astype(F32)
    spread = (
        lax.broadcasted_iota(jnp.int32, (heads, width), 0)
        == lax.broadcasted_iota(jnp.int32, (heads, width), 1) // dim
    ).astype(F32)
    lane = lax.broadcasted_iota(jnp.int32, (rows, 2 * dim), 1)
    for b in range(blocks):
        at = slice(b * rows, (b + 1) * rows)
        cum = exact(lower, log_decay[at, :])
        cum_t = exact(log_decay_t[:, at], upper)
        wide = exact(cum, spread)
        from_start = jnp.exp(wide)
        last = wide[rows - 1 : rows, :]
        start[at, :] = from_start
        end[at, :] = jnp.exp(last - wide)
        ends[b : b + 1, :] = jnp.exp(last)
        scaled[at, :] = (q[at, :].astype(F32) * from_start).astype(BF)
        for h in range(heads):
            pair = slice(h // 2 * 2 * dim, (h // 2 + 1) * 2 * dim)
            decay = jnp.where(
                causal, jnp.exp(jnp.minimum(cum[:, h : h + 1] - cum_t[h : h + 1, :], 0.0)), 0.0
            )
            decays[b, h] = decay
            own = jnp.where(lane // dim == h % 2, q[at, pair], jnp.zeros((), BF))
            scores[b, h] = (contract(own, k[at, pair], 1, 1) * decay).astype(BF)


def mix_body(blocks, heads, *refs):
    pieces = refs[:4]
    w_out, scaled, ends, grad_mix, message, later = refs[4:]
    place = lax.axis_index("tp")
    share = pieces[0].shape[1]
    total = None
    for m in range(4):
        at = pl.multiple_of((place ^ m) * share, share)
        term = contract(pieces[m][...], w_out[pl.ds(at, share), :], 1, 0)
        total = term if total is None else total + term
    grad = total.astype(BF)
    grad_mix[...] = grad
    rows = grad.shape[0] // blocks
    width = grad.shape[1]
    dim = width // heads
    lane = lax.broadcasted_iota(jnp.int32, (dim, 2 * dim), 1)
    running = None
    for b in reversed(range(blocks)):
        parts = []
        for p in range(heads // 2):
            at, pair = slice(b * rows, (b + 1) * rows), slice(p * 2 * dim, (p + 1) * 2 * dim)
            full = contract(scaled[at, pair], grad[at, pair], 0, 0)
            parts.append(jnp.where(lane < dim, full[:dim], full[dim:]))
        outer = jnp.concatenate(parts, axis=1)
        if b > 0:
            later[b - 1] = outer
        running = outer if running is None else ends[b : b + 1, :] * running + outer
    message[:dim, :] = running.astype(BF)
    factor = ends[0:1, :]
    for b in range(1, blocks):
        factor = factor * ends[b : b + 1, :]
    message[dim:, :] = jnp.broadcast_to(factor, (8, width)).astype(BF)


def paired(square, dim):
    both = jnp.concatenate([square, square], axis=0)
    row = lax.broadcasted_iota(jnp.int32, both.shape, 0)
    lane = lax.broadcasted_iota(jnp.int32, both.shape, 1)
    return jnp.where((row < dim) == (lane < dim), both, jnp.zeros((), both.dtype))


def local_body(blocks, heads, grad, q, k, v, decays, scores, start, states, out_q, key_in, value_in):
    rows = q.shape[0] // blocks
    dim = q.shape[1] // heads
    lane = lax.broadcasted_iota(jnp.int32, (rows, 2 * dim), 1)
    zero = jnp.zeros((), BF)
    for b in range(blocks):
        for p in range(heads // 2):
            at, pair = slice(b * rows, (b + 1) * rows), slice(p * 2 * dim, (p + 1) * 2 * dim)
            g, qq, kk, vv = grad[at, pair], q[at, pair], k[at, pair], v[at, pair]
            carry = contract(g, paired(states[b, :, pair], dim), 1, 1)
            to_q = carry * start[at, pair]
            to_k = to_v = None
            for i in range(2):
                mine = lane // dim == i
                g_own = jnp.where(mine, g, zero)
                weighted = (contract(g_own, vv, 1, 1) * decays[b, 2 * p + i]).astype(BF)
                to_q = to_q + contract(weighted, jnp.where(mine, kk, zero), 1, 0)
                a = contract(weighted, jnp.where(mine, qq, zero), 0, 0)
                c = contract(scores[b, 2 * p + i], g_own, 0, 0)
                to_k = a if to_k is None else to_k + a
                to_v = c if to_v is None else to_v + c
            out_q[at, pair] = to_q.astype(BF)
            key_in[at, pair] = to_k
            value_in[at, pair] = to_v


def pair_body(dim, own, other, out):
    upper = (lax.axis_index("sp") & 1) == 1
    mine, theirs = own[...].astype(F32), other[...].astype(F32)
    first = jnp.where(upper, theirs, mine)
    second = jnp.where(upper, mine, theirs)
    factor = first[dim : dim + 1, :]
    out[:dim, :] = (first[:dim, :] + factor * second[:dim, :]).astype(BF)
    out[dim:, :] = (first[dim:, :] * second[dim:, :]).astype(BF)


def carry_body(pairs, blocks, heads, *refs):
    other, messages = refs[0], refs[1 : 1 + pairs]
    k, v, key_in, value_in, end, ends, later, out_k, out_v, factors, weights = refs[1 + pairs :]
    place = lax.axis_index("sp") // 2
    upper = (lax.axis_index("sp") & 1) == 1
    rows = k.shape[0] // blocks
    width = k.shape[1]
    dim = width // heads
    for j in range(pairs):
        factors[pl.ds(place ^ j, 1), :] = messages[j][dim : dim + 1, :].astype(F32)
    running = jnp.where(upper, 1.0, other[dim : dim + 1, :].astype(F32))
    for u in range(pairs):
        ahead = u > place
        weights[pl.ds(place ^ u, 1), :] = jnp.where(ahead, running, 0.0)
        running = jnp.where(ahead, running * factors[u : u + 1, :], running)
    state = jnp.where(upper, 0.0, other[:dim, :].astype(F32))
    for j in range(1, pairs):
        state = state + weights[j : j + 1, :] * messages[j][:dim, :].astype(F32)
    for b in reversed(range(blocks)):
        carried = state.astype(BF)
        if b > 0:
            state = ends[b : b + 1, :] * state + later[b - 1]
        for p in range(heads // 2):
            at, pair = slice(b * rows, (b + 1) * rows), slice(p * 2 * dim, (p + 1) * 2 * dim)
            square = paired(carried[:, pair], dim)
            scale = end[at, pair]
            out_k[at, pair] = (
                key_in[at, pair] + contract(v[at, pair], square, 1, 1) * scale
            ).astype(BF)
            out_v[at, pair] = (
                value_in[at, pair] + contract(k[at, pair], square, 1, 0) * scale
            ).astype(BF)


def split_body(pairs, *refs):
    pieces, outs, full = refs[:4], refs[4 : 4 + pairs], refs[4 + pairs]
    tp, place = lax.axis_index("tp"), lax.axis_index("sp") // 2
    share = pieces[0].shape[1]
    half = full.shape[0]
    top = pl.multiple_of((tp & 1) * half, half)
    for m in range(4):
        at = pl.multiple_of((tp ^ m) * share, share)
        full[:, pl.ds(at, share)] = pieces[m][pl.ds(top, half), :]
    width = outs[0].shape[1]
    for j in range(pairs):
        at = pl.multiple_of((place ^ j) * width, width)
        outs[j][...] = full[:, pl.ds(at, width)]


def out_grad_body(pairs, own, other, *refs):
    mixers, (mine, theirs, hold) = refs[:pairs], refs[pairs:]
    half = own.shape[0] // pairs
    top = pl.multiple_of((lax.axis_index("tp") & 1) * half, half)
    low = pl.multiple_of((1 - (lax.axis_index("tp") & 1)) * half, half)
    left, right = [], []
    for j in range(pairs):
        at = slice(j * half, (j + 1) * half)
        left += [own[at, :], other[at, :]]
        right += [mixers[j][pl.ds(top, half), :], mixers[j][pl.ds(low, half), :]]
    hold[...] = contract(jnp.concatenate(left, axis=0), jnp.concatenate(right, axis=0), 0, 0)
    block = mine.shape[0]
    at = pl.multiple_of((lax.axis_index("sp") & 1) * block, block)
    away = pl.multiple_of((1 - (lax.axis_index("sp") & 1)) * block, block)
    mine[...] = hold[pl.ds(at, block), :]
    theirs[...] = hold[pl.ds(away, block), :].astype(BF)


def final_body(mine, got, out):
    out[...] = mine[...] + got[...].astype(F32)


def step(
    moe_input,
    cotangent,
    routes,
    route_weights,
    gate_weight,
    up_weight,
    down_weight,
    out_weight,
    mixer_output,
    queries,
    key_vectors,
    value_vectors,
    log_decay,
    block_states,
):
    tokens, width = cotangent.shape
    n = lax.axis_size("sp")
    cap = 5 * tokens * TOP_K // (4 * n)
    share = width // lax.axis_size("tp")
    hidden = gate_weight.shape[2]
    groups = [list(range(n // 2, n)), list(range(n // 2))]
    pairs = n // 2

    def over_sp(x, k):
        if k == 0:
            return x
        return lax.ppermute(x, "sp", [(i, i ^ k) for i in range(n)])

    def over_tp(x, m):
        return lax.ppermute(x, "tp", [(i, i ^ m) for i in range(4)])

    def spread_tp(x):
        across = over_tp(x, 2)
        return [x, over_tp(x, 1), across, over_tp(across, 1)]

    outs = kernel_call(
        functools.partial(dispatch_body, n, cap),
        [((cap, share), BF)] * (2 * n) + [((n * cap, tokens), BF)],
        (moe_input, cotangent, routes.T, route_weights.T),
        4 * n * cap * tokens * share,
        far=(0, 1),
        scratch=[pltpu.VMEM((tokens, share), BF)] * 2 + [pltpu.SemaphoreType.DMA((2,))],
    )
    pick_t = outs[2 * n].T

    order = [k for group in groups for k in group]
    x_in = {k: over_sp(outs[k], k) for k in order}
    y_in = {k: over_sp(outs[n + k], k) for k in order}
    xs = [spread_tp(jnp.concatenate([x_in[k] for k in group], axis=0)) for group in groups]
    ys = [spread_tp(jnp.concatenate([y_in[k] for k in group], axis=0)) for group in groups]

    heads = log_decay.shape[1]
    blocks = block_states.shape[0]
    dim = queries.shape[1] // heads
    rows = tokens // blocks
    local = queries.shape[1]
    decays, scores, scaled, start, end, ends = kernel_call(
        functools.partial(retention_pre_body, blocks),
        [
            ((blocks, heads, rows, rows), F32),
            ((blocks, heads, rows, rows), BF),
            ((tokens, local), BF),
            ((tokens, local), F32),
            ((tokens, local), F32),
            ((blocks, local), F32),
        ],
        (log_decay, log_decay.T, queries, key_vectors),
        10 * tokens * rows * local,
    )
    states = block_states.transpose(0, 2, 1, 3).reshape(blocks, dim, heads * dim)

    mixers = [over_sp(mixer_output, 2 * j) for j in range(pairs)]

    pres = []
    for g in range(len(groups)):
        count = xs[g][0].shape[0]
        pres.append(
            kernel_call(
                functools.partial(pre_body, g),
                [((count, hidden), F32)] * 2,
                (*xs[g], gate_weight, up_weight),
                4 * count * width * hidden,
            )
        )
    gate_grads, up_grads, acts, returned = [], [], [], {}
    for g, group in enumerate(groups):
        count = xs[g][0].shape[0]
        gate_grad, up_grad, act, near, far0, far1 = kernel_call(
            expert_body,
            [((count, hidden), BF)] * 3
            + [((2, count, share), BF), ((count, share), BF), ((count, share), BF)],
            (*ys[g], gate_weight, up_weight, down_weight, *pres[g]),
            6 * count * width * hidden,
        )
        gate_grads.append(gate_grad)
        up_grads.append(up_grad)
        acts.append(act)
        near_in = over_tp(near, 1)
        (send,) = kernel_call(near_sum_body, [((count, share), BF)], (far0, near_in), count * share)
        got = over_tp(send, 2)
        back = kernel_call(
            functools.partial(far_sum_body, cap, len(group)),
            [((cap, share), BF)] * len(group),
            (far1, near_in, got),
            3 * count * share,
        )
        for k, piece in zip(group, back):
            returned[k] = over_sp(piece, k)

    flat = [x for xg in xs for x in xg] + [y for yg in ys for y in yg]
    grad_gate, grad_up, grad_down = kernel_call(
        functools.partial(weight_grad_body, len(groups)),
        [((1, width, hidden), F32), ((1, width, hidden), F32), ((1, hidden, width), F32)],
        (*flat, *gate_grads, *up_grads, *acts),
        6 * n * cap * width * hidden,
        scratch=[pltpu.VMEM((12, share, hidden), F32), pltpu.SemaphoreType.DMA((12,))],
        far_out=True,
        vmem=24,
    )

    back_rows = [returned[k] for k in range(n)]
    (residual,) = kernel_call(
        functools.partial(combine_body, n, cap),
        [((tokens, share), BF)],
        (cotangent, pick_t, *back_rows),
        2 * n * cap * tokens * share,
        far=(0,),
        scratch=[pltpu.VMEM((tokens, share), BF), pltpu.SemaphoreType.DMA((1,))],
    )
    pieces = spread_tp(residual)
    block = width // n
    half = tokens // 2
    split = kernel_call(
        functools.partial(split_body, pairs),
        [((half, 2 * block), BF)] * pairs,
        pieces,
        tokens * width,
        scratch=[pltpu.VMEM((half, width), BF)],
    )
    own = jnp.concatenate([over_sp(split[j], 2 * j) for j in range(pairs)], axis=0)
    other = over_tp(own, 1)

    grad_mix, message, later = kernel_call(
        functools.partial(mix_body, blocks, heads),
        [((tokens, local), BF), ((dim + 8, local), BF), ((blocks - 1, dim, local), F32)],
        (*pieces, out_weight, scaled, ends),
        2 * tokens * width * local,
    )
    mate = over_sp(message, 1)
    (joined,) = kernel_call(
        functools.partial(pair_body, dim), [((dim + 8, local), BF)], (message, mate), dim * local
    )
    messages = [over_sp(joined, 2 * j) for j in range(pairs)]

    grad_queries, key_in, value_in = kernel_call(
        functools.partial(local_body, blocks, heads),
        [((tokens, local), BF), ((tokens, local), F32), ((tokens, local), F32)],
        (grad_mix, queries, key_vectors, value_vectors, decays, scores, start, states),
        20 * tokens * rows * local,
    )
    grad_keys, grad_values = kernel_call(
        functools.partial(carry_body, pairs, blocks, heads),
        [((tokens, local), BF)] * 2,
        (mate, *messages, key_vectors, value_vectors, key_in, value_in, end, ends, later),
        8 * tokens * dim * local,
        scratch=[pltpu.VMEM((pairs, local), F32), pltpu.VMEM((pairs, local), F32)],
    )
    columns = mixer_output.shape[1]
    mine, theirs = kernel_call(
        functools.partial(out_grad_body, pairs),
        [((block, columns), F32), ((block, columns), BF)],
        (own, other, *mixers),
        2 * n * tokens * block * columns,
        scratch=[pltpu.VMEM((2 * block, columns), F32)],
    )
    got = over_sp(theirs, 1)
    (grad_out,) = kernel_call(final_body, [((block, columns), F32)], (mine, got), block * columns)
    return (grad_gate, grad_up, grad_down, grad_out, grad_queries, grad_keys, grad_values)


def solution(mesh):
    return jax.shard_map(
        step,
        mesh=mesh,
        in_specs=(
            P("sp", None),
            P("sp", None),
            P("sp", None),
            P("sp", None),
            P("sp", None, "tp"),
            P("sp", None, "tp"),
            P("sp", "tp", None),
            P(None, "tp"),
            P("sp", "tp"),
            P("sp", "tp"),
            P("sp", "tp"),
            P("sp", "tp"),
            P("sp", "tp"),
            P("sp", "tp", None, None),
        ),
        out_specs=(
            P("sp", None, "tp"),
            P("sp", None, "tp"),
            P("sp", "tp", None),
            P("sp", "tp"),
            P("sp", "tp"),
            P("sp", "tp"),
            P("sp", "tp"),
        ),
        check_vma=False,
    )
```
